256 devices in a mesh: fs: 32 (over z, y), tp: 8 (over x, core).
Axes of the slice: x: 4, y: 4, z: 8, core: 2. Of those that a mesh axis runs over, the one named last changes fastest.
Arguments:
- inputs: bfloat16 [8192, 2048], P('fs', 'tp'), may hold values from -6 to 6
- cotangent: bfloat16 [8192, 2048], P('fs', 'tp'), may hold values from -8 to 8
- gate_weight: bfloat16 [2048, 5632], P('fs', 'tp'), may hold values from -0.125 to 0.125
- up_weight: bfloat16 [2048, 5632], P('fs', 'tp'), may hold values from -0.125 to 0.125
- down_weight: bfloat16 [5632, 2048], P('tp', 'fs'), may hold values from -0.078125 to 0.078125
Outputs:
- grad_inputs: bfloat16 [8192, 2048], P('fs', 'tp')
- grad_gate: float32 [2048, 5632], P('fs', 'tp')
- grad_up: float32 [2048, 5632], P('fs', 'tp')
- grad_down: float32 [5632, 2048], P('tp', 'fs')
The draws below stay inside these ranges and needn't reach their ends.
All inputs are finite; a program needn't handle non-finite values.
Results may differ from the reference program's by a relative error of at most 0.015.
Values may be sent and summed in bfloat16 or wider, within the bound.
No kernel may reach another device: no remote copies, remote signals or barrier semaphores. Data moves between devices by JAX's collectives and lax.ppermute only.
A program may use at most 64 MiB of HBM per device.

```python
import jax
import jax.numpy as jnp
from jax import lax

D = 2048
FF = 5632
TOKENS = 8192
N_TP = 8


def spiked(entries, own_key, source, target, blocks, factor):
    def block_of(axis_at):
        return (jnp.arange(entries.shape[axis_at]) // (entries.shape[axis_at] // blocks)).reshape((-1,) + (1,) * (entries.ndim - 1 - axis_at))

    near = jax.random.permutation(own_key, blocks)[block_of(target)]
    other_side = (block_of(target) + blocks // 2) % blocks
    return jnp.where((block_of(source) == near) | (block_of(source) == other_side), factor * entries, entries)


def levels(key, dims, cuts, smallest, high):
    level = 1.0
    for dim, blocks in cuts:
        steps = jax.random.uniform(jax.random.fold_in(jax.random.fold_in(key, 6), dim), (blocks,), jnp.float32, smallest / len(cuts), high / len(cuts))
        level = level * jnp.repeat(jnp.exp(steps), dims[dim] // blocks).reshape((-1,) + (1,) * (len(dims) - 1 - dim))
    return level


def scatter_about(own_key, extent, scale, most, split=(), kind=jnp.bfloat16):
    result = jax.random.normal(own_key, extent, jnp.float32) * scale
    if len(split) > 0:
        result = levels(own_key, extent, split, -0.22, 0.18) * result
    return jnp.clip(result, min=-most, max=most).astype(kind)


def heavy_noise(rng, shape, scale, bound, pieces, heavy, kind=jnp.bfloat16):
    entries = scale * jax.random.normal(rng, shape, jnp.float32)
    if pieces:
        entries = entries * levels(rng, shape, pieces, -0.22, 0.18)
    return jnp.clip(spiked(entries, jax.random.fold_in(rng, 3), *heavy), -bound, bound).astype(kind)


def setup_inputs(seed: int = 0) -> dict:
    keys = jax.random.split(jax.random.key(seed), 6)
    inputs = scatter_about(keys[0], (TOKENS, D), 1.0, 6.0, ((0, 32), (1, 8)))
    cotangent = heavy_noise(keys[1], (TOKENS, D), 1.0, 8.0, ((0, 32), (1, 8)), (0, 1, 32, 2.75))
    gate_weight = scatter_about(keys[2], (D, FF), D ** -0.5, 0.125, ((0, 32), (1, 8)))
    up_weight = scatter_about(keys[3], (D, FF), D ** -0.5, 0.125, ((0, 32), (1, 8)))
    down_weight = scatter_about(keys[4], (FF, D), FF ** -0.5, 0.078125, ((0, 8), (1, 32)))
    return {"inputs": inputs, "cotangent": cotangent, "gate_weight": gate_weight, "up_weight": up_weight, "down_weight": down_weight}


def contract_rows(left, right):
    return lax.dot_general(left, right, (((0,), (0,)), ((), ())), preferred_element_type=jnp.float32)


def contract_cols(left, right):
    return lax.dot_general(left, right, (((1,), (1,)), ((), ())), preferred_element_type=jnp.float32)


def reference(inputs, cotangent, gate_weight, up_weight, down_weight):
    gate_pre = jnp.dot(inputs, gate_weight, preferred_element_type=jnp.float32)
    up_pre = jnp.dot(inputs, up_weight, preferred_element_type=jnp.float32)
    gate_sig = jax.nn.sigmoid(gate_pre)
    gate_act = gate_pre * gate_sig
    hidden = (gate_act * up_pre).astype(jnp.bfloat16)
    grad_hidden = contract_cols(cotangent, down_weight)
    grad_gate_pre = (grad_hidden * up_pre * gate_sig * (1.0 + gate_pre * (1.0 - gate_sig))).astype(jnp.bfloat16)
    grad_up_pre = (grad_hidden * gate_act).astype(jnp.bfloat16)
    grad_gate = contract_rows(inputs, grad_gate_pre)
    grad_up = contract_rows(inputs, grad_up_pre)
    grad_down = contract_rows(hidden, cotangent)
    width = FF // N_TP

    def add_block(block_index, running):
        offset = (block_index * width).astype(jnp.int32)
        block_gate = lax.dynamic_slice_in_dim(grad_gate_pre, offset, width, 1)
        block_up = lax.dynamic_slice_in_dim(grad_up_pre, offset, width, 1)
        weight_gate = lax.dynamic_slice_in_dim(gate_weight, offset, width, 1)
        weight_up = lax.dynamic_slice_in_dim(up_weight, offset, width, 1)
        partial_sum = contract_cols(block_gate, weight_gate) + contract_cols(block_up, weight_up)
        rounded = lax.optimization_barrier(partial_sum.astype(jnp.bfloat16))
        return running + rounded.astype(jnp.float32)

    summed = lax.fori_loop(0, N_TP, add_block, jnp.zeros(inputs.shape, jnp.float32))
    grad_inputs = summed.astype(jnp.bfloat16)
    return (grad_inputs, grad_gate, grad_up, grad_down)
```

```python
import jax
import jax.numpy as jnp
from jax import lax
from jax.experimental import pallas as pl
from jax.experimental.pallas import tpu as pltpu
from jax.sharding import Mesh
from jax.sharding import PartitionSpec as P


NZ, NY, NX = 8, 4, 4
BLOCK = 176
HALF = 128
SWAP = [(0, 1), (1, 0)]
FULL = pl.BlockSpec(memory_space=pltpu.VMEM)


def dot_nt(left, right):
    return lax.dot_general(
        left, right, (((1,), (1,)), ((), ())), preferred_element_type=jnp.float32
    )


def dot_nn(left, right):
    return lax.dot_general(
        left, right, (((1,), (0,)), ((), ())), preferred_element_type=jnp.float32
    )


def dot_tn(left, right):
    return lax.dot_general(
        left, right, (((0,), (0,)), ((), ())), preferred_element_type=jnp.float32
    )


def forward_kernel(acts, weights_a, weights_b, acts_out, hid_out, grads_out):
    for which in range(2):
        for y in range(NY):
            acts_out[which, y * HALF : (y + 1) * HALF, :] = acts[
                which * HALF : (which + 1) * HALF, y * 2048 : (y + 1) * 2048
            ]
    for which, weights in ((0, weights_a), (1, weights_b)):
        gate_pre = dot_nt(acts_out[0], weights[0:BLOCK, :])
        up_pre = dot_nt(acts_out[0], weights[BLOCK : 2 * BLOCK, :])
        grad_hidden = dot_nt(acts_out[1], weights[2 * BLOCK : 3 * BLOCK, :])
        gate_sig = jax.nn.sigmoid(gate_pre)
        gate_act = gate_pre * gate_sig
        hid_out[which, 0] = (
            grad_hidden * up_pre * gate_sig * (1.0 + gate_pre * (1.0 - gate_sig))
        ).astype(jnp.bfloat16)
        hid_out[which, 1] = (grad_hidden * gate_act).astype(jnp.bfloat16)
        hid_out[which, 2] = (gate_act * up_pre).astype(jnp.bfloat16)
    for part, which in ((0, 0), (1, 0), (2, 1)):
        for z in range(NZ):
            grads_out[z, part * BLOCK : (part + 1) * BLOCK, :] = dot_tn(
                hid_out[0, part], acts_out[which, :, z * 256 : (z + 1) * 256]
            ).astype(jnp.bfloat16)


def inputs_kernel(hid, weights_a, weights_b, out):
    for x in range(NX):
        total = jnp.zeros((NY * HALF, 512), jnp.float32)
        for which, weights in ((0, weights_a), (1, weights_b)):
            for part in range(2):
                total = total + dot_nn(
                    hid[which, part],
                    weights[part * BLOCK : (part + 1) * BLOCK, x * 512 : (x + 1) * 512],
                )
        for y in range(NY):
            out[y * NX + x] = total[y * HALF : (y + 1) * HALF].astype(jnp.bfloat16)


def weights_kernel(hid, acts, other, out):
    for part, which in ((0, 0), (1, 0), (2, 1)):
        for z in range(NZ):
            rows = slice(part * BLOCK, (part + 1) * BLOCK)
            own = dot_tn(hid[1, part], acts[which, :, z * 256 : (z + 1) * 256])
            out[z, rows, :] = (own + other[z, rows, :].astype(jnp.float32)).astype(jnp.bfloat16)


def call(kernel, outs, *args):
    shapes = [jax.ShapeDtypeStruct(s, jnp.bfloat16) for s in outs]
    return pl.pallas_call(
        kernel,
        out_shape=shapes,
        in_specs=[FULL] * len(args),
        out_specs=[FULL] * len(outs),
        compiler_params=pltpu.CompilerParams(vmem_limit_bytes=56 * 1024 * 1024),
    )(*args)


def per_device(inputs, cotangent, gate_weight, up_weight, down_weight):
    core = lax.axis_index("core")

    both = jnp.stack([inputs, cotangent]).reshape(2, 2, HALF, 256)
    kept = lax.dynamic_index_in_dim(both, core, 1, keepdims=False)
    sent = lax.dynamic_index_in_dim(both, 1 - core, 1, keepdims=False)
    came = lax.ppermute(sent, "core", SWAP)
    mine = jnp.where(
        core == 0,
        jnp.concatenate([kept, came], axis=2),
        jnp.concatenate([came, kept], axis=2),
    ).reshape(2 * HALF, 512)
    acts_flat = lax.all_gather(mine, ("y", "x"), axis=1, tiled=True)

    stacked = jnp.stack([gate_weight.T, up_weight.T, down_weight])
    pieces = stacked.reshape(3, NY, BLOCK, 64).transpose(1, 0, 2, 3).reshape(NY, 3 * BLOCK, 64)
    rows = lax.all_to_all(pieces, "y", split_axis=0, concat_axis=0, tiled=True)
    rows = rows.transpose(1, 0, 2).reshape(3 * BLOCK, 256)
    w_own = lax.all_gather(rows, "z", axis=1, tiled=True)
    w_other = lax.ppermute(w_own, "core", SWAP)

    acts, hid, grads_other = call(
        forward_kernel,
        [(2, NY * HALF, 2048), (2, 3, NY * HALF, BLOCK), (NZ, 3 * BLOCK, 256)],
        acts_flat,
        w_other,
        w_own,
    )
    grads_came = lax.ppermute(grads_other, "core", SWAP)
    (partial_inputs,) = call(inputs_kernel, [(NY * NX, HALF, 512)], hid, w_other, w_own)
    (grads,) = call(weights_kernel, [(NZ, 3 * BLOCK, 256)], hid, acts, grads_came)

    summed = lax.psum_scatter(grads, "z", scatter_dimension=0, tiled=True)
    summed = summed.reshape(3 * BLOCK, NY, 64).transpose(1, 0, 2)
    blocks = lax.all_to_all(summed, "y", split_axis=0, concat_axis=0, tiled=True)
    blocks = blocks.reshape(NY, 3, BLOCK, 64).transpose(1, 0, 2, 3).reshape(3, NY * BLOCK, 64)
    blocks = blocks.astype(jnp.float32)

    arrived = lax.all_to_all(partial_inputs, ("y", "x"), split_axis=0, concat_axis=0, tiled=True)
    total = arrived.astype(jnp.float32).sum(axis=0).astype(jnp.bfloat16).reshape(HALF, 2, 256)
    keep = lax.dynamic_index_in_dim(total, core, 1, keepdims=False)
    give = lax.dynamic_index_in_dim(total, 1 - core, 1, keepdims=False)
    take = lax.ppermute(give, "core", SWAP)
    grad_inputs = jnp.where(
        core == 0,
        jnp.concatenate([keep, take], axis=0),
        jnp.concatenate([take, keep], axis=0),
    )
    return grad_inputs, blocks[0].T, blocks[1].T, blocks[2]


def solution(mesh):
    finer = Mesh(mesh.devices.reshape(NZ, NY, NX, 2), ("z", "y", "x", "core"))
    fs, tp = ("z", "y"), ("x", "core")
    return jax.shard_map(
        per_device,
        mesh=finer,
        in_specs=(P(fs, tp), P(fs, tp), P(fs, tp), P(fs, tp), P(tp, fs)),
        out_specs=(P(fs, tp), P(fs, tp), P(fs, tp), P(tp, fs)),
        check_vma=False,
    )
```

```python
import jax
import jax.numpy as jnp
from jax import lax
from jax.experimental import pallas as pl
from jax.experimental.pallas import tpu as pltpu
from jax.sharding import Mesh
from jax.sharding import PartitionSpec as P


NZ, NY, NX = 8, 4, 4
RING = 4
BLOCK = 176
COLS = 3 * BLOCK
HALF = 128
ROWS = NY * HALF
SWAP = [(0, 1), (1, 0)]
ORDER = (0, -1, 1, 2)
VMEM = pl.BlockSpec(memory_space=pltpu.VMEM)
SMEM = pl.BlockSpec(memory_space=pltpu.SMEM)
ANY = pl.BlockSpec(memory_space=pl.ANY)


def dot(left, right, dims):
    return lax.dot_general(
        left, right, (dims, ((), ())), preferred_element_type=jnp.float32
    )


def call(kernel, outs, specs, *args, dtype=jnp.bfloat16, scratch=(), aliases={}, out_specs=None):
    return pl.pallas_call(
        kernel,
        out_shape=[jax.ShapeDtypeStruct(s, dtype) for s in outs],
        in_specs=specs,
        out_specs=out_specs or [VMEM] * len(outs),
        scratch_shapes=[pltpu.VMEM(s, jnp.bfloat16) for s in scratch],
        input_output_aliases=aliases,
        compiler_params=pltpu.CompilerParams(vmem_limit_bytes=56 * 1024 * 1024),
    )(*args)


def shift(array, axis, by):
    return lax.ppermute(array, axis, [(i, (i + by) % RING) for i in range(RING)])


def around(own, axis):
    return own, shift(own, axis, 1), shift(own, axis, -1), shift(own, axis, 2)


def around_in_halves(own, axis):
    low, high = shift(own, axis, 1), shift(own, axis, -1)
    far_first = shift(low[:2], axis, 1)
    far_last = shift(high[2:], axis, -1)
    return own, low, high, far_first, far_last


def front_kernel(
    place, gate, up, down, inputs, cotangent, came, keep, to_next, to_prev, to_far, inp, cot, pieces
):
    for y in range(NY):
        for part, array in enumerate((gate, up, down)):
            pieces[y, :, part * BLOCK : (part + 1) * BLOCK] = array[
                :, y * BLOCK : (y + 1) * BLOCK
            ]
    for out, by in ((keep, 0), (to_next, 1), (to_prev, NY - 1), (to_far, 2)):
        out[...] = pieces[(place[0] + by) % NY]
    for core in range(2):

        @pl.when(place[2] == core)
        def _():
            own = slice(core * 256, (core + 1) * 256)
            other = slice((1 - core) * 256, (2 - core) * 256)
            for which, (array, out) in enumerate(((inputs, inp), (cotangent, cot))):
                out[:, own] = array[core * HALF : (core + 1) * HALF, :]
                out[:, other] = came[which]


def join_kernel(place, kept, from_prev, from_next, from_far, out, pieces):
    for array, by in ((kept, 0), (from_prev, NY - 1), (from_next, 1), (from_far, 2)):
        pieces[(place[0] + by) % NY] = array[...]
    rows = jnp.concatenate([pieces[y] for y in range(NY)], axis=0)
    out[...] = rows.T


def split_kernel(place, grads, keep, to_next, to_prev, to_far, pieces):
    rows = grads[...].T
    for y in range(NY):
        pieces[y] = rows[y * 64 : (y + 1) * 64]
    for out, by in ((keep, 0), (to_next, 1), (to_prev, NY - 1), (to_far, 2)):
        out[...] = pieces[(place[0] + by) % NY]


def finish_kernel(place, kept, from_prev, from_next, from_far, gate, up, down, pieces):
    for array, by in ((kept, 0), (from_prev, NY - 1), (from_next, 1), (from_far, 2)):
        pieces[(place[0] + by) % NY] = array[...]
    for y in range(NY):
        for part, out in enumerate((gate, up, down)):
            out[:, y * BLOCK : (y + 1) * BLOCK] = pieces[
                y, :, part * BLOCK : (part + 1) * BLOCK
            ].astype(jnp.float32)


def exchange(pieces):
    keep, to_next, to_prev, to_far = pieces
    return keep, shift(to_next, "y", 1), shift(to_prev, "y", -1), shift(to_far, "y", 2)


def main_kernel(place, *refs):
    inp, cot = refs[0:5], refs[5:10]
    weights = refs[10:12]
    hid, grads_other, grads_own, acts, whole, flipped = refs[12:18]
    spots = ((0, 0, 4), (3, 0, 4), (1, 0, 4), (2, 0, 2), (2, 2, 4))
    for which, arrays in enumerate((inp, cot)):
        for array, (by, first, last) in zip(arrays, spots):
            for slot in range(first, last):
                near, far = place[1 - which] + ORDER[slot] + RING, place[which] + by
                x, y = (near, far) if which == 0 else (far, near)
                acts[
                    which,
                    pl.ds(pl.multiple_of((y % NY) * HALF, HALF), HALF),
                    pl.ds(pl.multiple_of((x % NX) * 512, 512), 512),
                ] = array[slot - first]
    for block, array in enumerate(weights):
        for z in range(NZ):
            whole[:, z * 256 : (z + 1) * 256] = array[z]
        gate_pre = dot(acts[0], whole[0:BLOCK, :], ((1,), (1,)))
        up_pre = dot(acts[0], whole[BLOCK : 2 * BLOCK, :], ((1,), (1,)))
        grad_hidden = dot(acts[1], whole[2 * BLOCK :, :], ((1,), (1,)))
        gate_sig = jax.nn.sigmoid(gate_pre)
        gate_act = gate_pre * gate_sig
        hid[block, 0] = (
            grad_hidden * up_pre * gate_sig * (1.0 + gate_pre * (1.0 - gate_sig))
        ).astype(jnp.bfloat16)
        hid[block, 1] = (grad_hidden * gate_act).astype(jnp.bfloat16)
        hid[block, 2] = (gate_act * up_pre).astype(jnp.bfloat16)
        for part in range(3):
            flipped[block, part] = hid[block, part].T

    def step(z, carry):
        lanes = pl.ds(pl.multiple_of(z * 256, 256), 256)
        for block, out in enumerate((grads_other, grads_own)):
            for part, which in ((0, 0), (1, 0), (2, 1)):
                out[z, part * BLOCK : (part + 1) * BLOCK, :] = dot(
                    flipped[block, part], acts[which, :, lanes], ((1,), (0,))
                ).astype(jnp.bfloat16)
        return carry

    lax.fori_loop(0, NZ, step, 0)


def inputs_kernel(hid, weights_a, weights_b, out):
    for z in range(NZ):
        total = jnp.zeros((ROWS, 256), jnp.float32)
        for block, array in enumerate((weights_a, weights_b)):
            for part in range(2):
                total = total + dot(
                    hid[block, part],
                    array[z, part * BLOCK : (part + 1) * BLOCK, :],
                    ((1,), (0,)),
                )
        for y in range(NY):
            out[y * NX + z // 2, :, (z % 2) * 256 : (z % 2 + 1) * 256] = total[
                y * HALF : (y + 1) * HALF
            ].astype(jnp.bfloat16)


def add_kernel(own, other, partial, out, partial_out):
    del partial, partial_out
    out[...] = (own[...].astype(jnp.float32) + other[...].astype(jnp.float32)).astype(jnp.bfloat16)


def hold_kernel(*refs):
    del refs


def per_device(inputs, cotangent, gate_weight, up_weight, down_weight):
    core = lax.axis_index("core")
    place = jnp.stack([lax.axis_index("y"), lax.axis_index("x"), core]).astype(jnp.int32)

    both = jnp.stack([inputs, cotangent]).reshape(2, 2, HALF, 256)
    sent = jnp.where(core == 0, both[:, 1], both[:, 0])
    came = lax.ppermute(sent, "core", SWAP)

    piece = (64, COLS)
    *pieces, inp, cot = call(
        front_kernel,
        [piece] * 4 + [(HALF, 512)] * 2,
        [SMEM] + [VMEM] * 6,
        place,
        gate_weight,
        up_weight,
        down_weight.T,
        inputs,
        cotangent,
        came,
        scratch=[(NY, *piece)],
    )

    moved = exchange(pieces)
    (rows,) = call(
        join_kernel,
        [(COLS, 256)],
        [SMEM] + [VMEM] * 4,
        place,
        *moved,
        scratch=[(NY, *piece)],
    )
    w_own = lax.all_gather(rows, "z", axis=0, tiled=False)

    inp_near, cot_near = around(inp, "x"), around(cot, "y")
    inp_blocks = around_in_halves(jnp.stack(inp_near), "y")
    cot_blocks = around_in_halves(jnp.stack(cot_near), "x")

    held = call(
        hold_kernel,
        [(NZ, COLS, 256)],
        [ANY] * 5,
        w_own,
        *inp_blocks[1:3],
        *cot_blocks[1:3],
        aliases={0: 0},
        out_specs=[ANY],
    )
    w_own = held[0]
    w_other = lax.ppermute(w_own, "core", SWAP)

    hid, grads_other, grads_own = call(
        main_kernel,
        [(2, 3, ROWS, BLOCK), (NZ, COLS, 256), (NZ, COLS, 256)],
        [SMEM] + [VMEM] * 12,
        place,
        *inp_blocks,
        *cot_blocks,
        w_other,
        w_own,
        scratch=[(2, ROWS, 2048), (COLS, 2048), (2, 3, BLOCK, ROWS)],
    )
    grads_came = lax.ppermute(grads_other, "core", SWAP)
    (partial,) = call(
        inputs_kernel, [(NY * NX, HALF, 512)], [VMEM] * 3, hid, w_other, w_own
    )
    grads, partial = call(
        add_kernel,
        [(NZ, COLS, 256), (NY * NX, HALF, 512)],
        [VMEM, VMEM, ANY],
        grads_own,
        grads_came,
        partial,
        aliases={2: 1},
        out_specs=[VMEM, ANY],
    )

    summed = lax.psum_scatter(grads, "z", scatter_dimension=0, tiled=False)
    pieces = call(
        split_kernel, [piece] * 4, [SMEM, VMEM], place, summed, scratch=[(NY, *piece)]
    )
    grad_gate, grad_up, grad_down = call(
        finish_kernel,
        [(64, NY * BLOCK)] * 3,
        [SMEM] + [VMEM] * 4,
        place,
        *exchange(pieces),
        dtype=jnp.float32,
        scratch=[(NY, *piece)],
    )

    arrived = lax.all_to_all(partial, ("y", "x"), split_axis=0, concat_axis=0, tiled=True)
    total = arrived.astype(jnp.float32).sum(axis=0).astype(jnp.bfloat16)
    lower, upper = total[:, :256], total[:, 256:]
    keep, give = jnp.where(core == 0, lower, upper), jnp.where(core == 0, upper, lower)
    take = lax.ppermute(give, "core", SWAP)
    grad_inputs = jnp.concatenate(
        [jnp.where(core == 0, keep, take), jnp.where(core == 0, take, keep)], axis=0
    )
    return grad_inputs, grad_gate, grad_up, grad_down.T


def solution(mesh):
    finer = Mesh(mesh.devices.reshape(NZ, NY, NX, 2), ("z", "y", "x", "core"))
    fs, tp = ("z", "y"), ("x", "core")

    return jax.shard_map(
        per_device,
        mesh=finer,
        in_specs=(P(fs, tp), P(fs, tp), P(fs, tp), P(fs, tp), P(tp, fs)),
        out_specs=(P(fs, tp), P(fs, tp), P(fs, tp), P(tp, fs)),
        check_vma=False,
    )
```

```python
import jax
import jax.numpy as jnp
from jax import lax
from jax.experimental import pallas as pl
from jax.experimental.pallas import tpu as pltpu
from jax.sharding import Mesh
from jax.sharding import PartitionSpec as P


NZ, NY, NX = 8, 4, 4
RING = 4
BLOCK = 176
COLS = 3 * BLOCK
HALF = 128
ROWS = NY * HALF
SWAP = [(0, 1), (1, 0)]
ORDER = (0, -1, 1, 2)
VMEM = pl.BlockSpec(memory_space=pltpu.VMEM)
SMEM = pl.BlockSpec(memory_space=pltpu.SMEM)
ANY = pl.BlockSpec(memory_space=pl.ANY)


def dot(left, right, dims):
    return lax.dot_general(
        left, right, (dims, ((), ())), preferred_element_type=jnp.float32
    )


def call(kernel, outs, specs, *args, dtype=jnp.bfloat16, scratch=(), sems=(), aliases={}, out_specs=None):
    return pl.pallas_call(
        kernel,
        out_shape=[jax.ShapeDtypeStruct(s, dtype) for s in outs],
        in_specs=specs,
        out_specs=out_specs or [VMEM] * len(outs),
        scratch_shapes=[pltpu.VMEM(s, jnp.bfloat16) for s in scratch]
        + [pltpu.SemaphoreType.DMA(s) for s in sems],
        input_output_aliases=aliases,
        compiler_params=pltpu.CompilerParams(vmem_limit_bytes=56 * 1024 * 1024),
    )(*args)


def shift(array, axis, by):
    return lax.ppermute(array, axis, [(i, (i + by) % RING) for i in range(RING)])


def around(own, axis):
    return own, shift(own, axis, 1), shift(own, axis, -1), shift(own, axis, 2)


def around_in_halves(own, axis):
    low, high = shift(own, axis, 1), shift(own, axis, -1)
    far_first = shift(low[:2], axis, 1)
    far_last = shift(high[2:], axis, -1)
    return own, low, high, far_first, far_last


def cut_kernel(place, gate, up, down, keep, to_next, to_prev, to_far, pieces):
    for y in range(NY):
        for part, array in enumerate((gate, up, down)):
            pieces[y, :, part * BLOCK : (part + 1) * BLOCK] = array[
                :, y * BLOCK : (y + 1) * BLOCK
            ]
    for out, by in ((keep, 0), (to_next, 1), (to_prev, NY - 1), (to_far, 2)):
        out[...] = pieces[(place[0] + by) % NY]


def pair_kernel(place, inputs, cotangent, came, inp, cot):
    for core in range(2):

        @pl.when(place[2] == core)
        def _():
            own = slice(core * 256, (core + 1) * 256)
            other = slice((1 - core) * 256, (2 - core) * 256)
            for which, (array, out) in enumerate(((inputs, inp), (cotangent, cot))):
                out[:, own] = array[core * HALF : (core + 1) * HALF, :]
                out[:, other] = came[which]


def join_kernel(place, kept, from_prev, from_next, from_far, out, pieces):
    for array, by in ((kept, 0), (from_prev, NY - 1), (from_next, 1), (from_far, 2)):
        pieces[(place[0] + by) % NY] = array[...]
    rows = jnp.concatenate([pieces[y] for y in range(NY)], axis=0)
    out[...] = rows.T


def split_kernel(place, grads, keep, to_next, to_prev, to_far, pieces):
    rows = grads[...].T
    for y in range(NY):
        pieces[y] = rows[y * 64 : (y + 1) * 64]
    for out, by in ((keep, 0), (to_next, 1), (to_prev, NY - 1), (to_far, 2)):
        out[...] = pieces[(place[0] + by) % NY]


def finish_kernel(place, kept, from_prev, from_next, from_far, gate, up, down, pieces):
    for array, by in ((kept, 0), (from_prev, NY - 1), (from_next, 1), (from_far, 2)):
        pieces[(place[0] + by) % NY] = array[...]
    for y in range(NY):
        for part, out in enumerate((gate, up, down)):
            out[:, y * BLOCK : (y + 1) * BLOCK] = pieces[
                y, :, part * BLOCK : (part + 1) * BLOCK
            ].astype(jnp.float32)


def exchange(pieces):
    keep, to_next, to_prev, to_far = pieces
    return keep, shift(to_next, "y", 1), shift(to_prev, "y", -1), shift(to_far, "y", 2)


def main_kernel(place, *refs):
    inp, cot = refs[0:5], refs[5:10]
    weights = refs[10:12]
    hid, grads_other, grads_own = refs[12:15]
    acts, whole, flipped, hid_at, out_at, acts_sems, weight_sems, out_sems = refs[15:]

    loads = []
    spots = ((0, 0, 4), (3, 0, 4), (1, 0, 4), (2, 0, 2), (2, 2, 4))
    for which, arrays in enumerate((inp, cot)):
        count = 0
        for array, (by, first, last) in zip(arrays, spots):
            for slot in range(first, last):
                near, far = place[1 - which] + ORDER[slot] + RING, place[which] + by
                x, y = (near, far) if which == 0 else (far, near)
                spot = acts.at[
                    which,
                    pl.ds(pl.multiple_of((y % NY) * HALF, HALF), HALF),
                    pl.ds(pl.multiple_of((x % NX) * 512, 512), 512),
                ]
                sem = acts_sems.at[which, count]
                loads.append(pltpu.make_async_copy(array.at[slot - first], spot, sem))
                count += 1
    fetches = [
        [
            pltpu.make_async_copy(
                array.at[z], whole.at[block, :, z * 256 : (z + 1) * 256], weight_sems.at[block, z]
            )
            for z in range(NZ)
        ]
        for block, array in enumerate(weights)
    ]
    for copy in loads + fetches[1] + fetches[0]:
        copy.start()
    for copy in loads:
        copy.wait()
    stores = []
    for block in (1, 0):
        for copy in fetches[block]:
            copy.wait()
        gate_pre = dot(acts[0], whole[block, 0:BLOCK, :], ((1,), (1,)))
        up_pre = dot(acts[0], whole[block, BLOCK : 2 * BLOCK, :], ((1,), (1,)))
        grad_hidden = dot(acts[1], whole[block, 2 * BLOCK :, :], ((1,), (1,)))
        gate_sig = jax.nn.sigmoid(gate_pre)
        gate_act = gate_pre * gate_sig
        hid_at[block, 0] = (
            grad_hidden * up_pre * gate_sig * (1.0 + gate_pre * (1.0 - gate_sig))
        ).astype(jnp.bfloat16)
        hid_at[block, 1] = (grad_hidden * gate_act).astype(jnp.bfloat16)
        hid_at[block, 2] = (gate_act * up_pre).astype(jnp.bfloat16)
        store = pltpu.make_async_copy(hid_at.at[block], hid.at[block], out_sems.at[block])
        store.start()
        stores.append(store)
        for part in range(3):
            flipped[block, part] = hid_at[block, part].T
    for block, out in ((1, grads_own), (0, grads_other)):

        def step(z, carry):
            lanes = pl.ds(pl.multiple_of(z * 256, 256), 256)
            for part, which in ((0, 0), (1, 0), (2, 1)):
                out_at[block, z, part * BLOCK : (part + 1) * BLOCK, :] = dot(
                    flipped[block, part], acts[which, :, lanes], ((1,), (0,))
                ).astype(jnp.bfloat16)
            return carry

        lax.fori_loop(0, NZ, step, 0)
        store = pltpu.make_async_copy(out_at.at[block], out, out_sems.at[2 + block])
        store.start()
        stores.append(store)
    for store in stores:
        store.wait()


def inputs_kernel(hid, weights_a, weights_b, out):
    for z in range(NZ):
        total = jnp.zeros((ROWS, 256), jnp.float32)
        for block, array in enumerate((weights_a, weights_b)):
            for part in range(2):
                total = total + dot(
                    hid[block, part],
                    array[z, part * BLOCK : (part + 1) * BLOCK, :],
                    ((1,), (0,)),
                )
        for y in range(NY):
            out[y * NX + z // 2, :, (z % 2) * 256 : (z % 2 + 1) * 256] = total[
                y * HALF : (y + 1) * HALF
            ].astype(jnp.bfloat16)


def hold_kernel(*refs):
    del refs


def per_device(inputs, cotangent, gate_weight, up_weight, down_weight):
    core = lax.axis_index("core")
    place = jnp.stack([lax.axis_index("y"), lax.axis_index("x"), core]).astype(jnp.int32)

    both = jnp.stack([inputs, cotangent]).reshape(2, 2, HALF, 256)
    sent = jnp.where(core == 0, both[:, 1], both[:, 0])
    came = lax.ppermute(sent, "core", SWAP)

    piece = (64, COLS)
    pieces = call(
        cut_kernel,
        [piece] * 4,
        [SMEM] + [VMEM] * 3,
        place,
        gate_weight,
        up_weight,
        down_weight.T,
        scratch=[(NY, *piece)],
    )
    moved = exchange(pieces)
    (rows,) = call(
        join_kernel,
        [(COLS, 256)],
        [SMEM] + [VMEM] * 4,
        place,
        *moved,
        scratch=[(NY, *piece)],
    )
    w_own = lax.all_gather(rows, "z", axis=0, tiled=False)

    inp, cot = call(
        pair_kernel, [(HALF, 512)] * 2, [SMEM] + [VMEM] * 3, place, inputs, cotangent, came
    )
    inp_near = around(inp, "x")
    cot_near = around(cot, "y")
    inp_blocks = around_in_halves(jnp.stack(inp_near), "y")
    cot_blocks = around_in_halves(jnp.stack(cot_near), "x")

    (w_own,) = call(
        hold_kernel,
        [(NZ, COLS, 256)],
        [ANY] * 5,
        w_own,
        *inp_blocks[1:3],
        *cot_blocks[1:3],
        aliases={0: 0},
        out_specs=[ANY],
    )
    w_other = lax.ppermute(w_own, "core", SWAP)

    grads_shape = (NZ, COLS, 256)
    hid_shape = (2, 3, ROWS, BLOCK)
    hid, grads_other, grads_own = call(
        main_kernel,
        [hid_shape, grads_shape, grads_shape],
        [SMEM] + [ANY] * 12,
        place,
        *inp_blocks,
        *cot_blocks,
        w_other,
        w_own,
        scratch=[
            (2, ROWS, 2048),
            (2, COLS, 2048),
            (2, 3, BLOCK, ROWS),
            hid_shape,
            (2, *grads_shape),
        ],
        sems=[(2, 16), (2, NZ), (4,)],
        out_specs=[ANY] * 3,
    )
    grads_came = lax.ppermute(grads_other, "core", SWAP)
    (partial,) = call(
        inputs_kernel, [(NY * NX, HALF, 512)], [VMEM] * 3, hid, w_other, w_own
    )
    grads = (grads_own.astype(jnp.float32) + grads_came.astype(jnp.float32)).astype(jnp.bfloat16)
    (partial,) = call(
        hold_kernel,
        [(NY * NX, HALF, 512)],
        [ANY] * 2,
        partial,
        grads,
        aliases={0: 0},
        out_specs=[ANY],
    )

    summed = lax.psum_scatter(grads, "z", scatter_dimension=0, tiled=False)
    pieces = call(
        split_kernel, [piece] * 4, [SMEM, VMEM], place, summed, scratch=[(NY, *piece)]
    )
    grad_gate, grad_up, grad_down = call(
        finish_kernel,
        [(64, NY * BLOCK)] * 3,
        [SMEM] + [VMEM] * 4,
        place,
        *exchange(pieces),
        dtype=jnp.float32,
        scratch=[(NY, *piece)],
    )

    arrived = lax.all_to_all(partial, ("y", "x"), split_axis=0, concat_axis=0, tiled=True)
    total = arrived.astype(jnp.float32).sum(axis=0).astype(jnp.bfloat16)
    lower, upper = total[:, :256], total[:, 256:]
    keep, give = jnp.where(core == 0, lower, upper), jnp.where(core == 0, upper, lower)
    take = lax.ppermute(give, "core", SWAP)
    grad_inputs = jnp.concatenate(
        [jnp.where(core == 0, keep, take), jnp.where(core == 0, take, keep)], axis=0
    )
    return grad_inputs, grad_gate, grad_up, grad_down.T


def solution(mesh):
    finer = Mesh(mesh.devices.reshape(NZ, NY, NX, 2), ("z", "y", "x", "core"))
    fs, tp = ("z", "y"), ("x", "core")

    return jax.shard_map(
        per_device,
        mesh=finer,
        in_specs=(P(fs, tp), P(fs, tp), P(fs, tp), P(fs, tp), P(tp, fs)),
        out_specs=(P(fs, tp), P(fs, tp), P(fs, tp), P(tp, fs)),
        check_vma=False,
    )
```

```python
import jax
import jax.numpy as jnp
from jax import lax
from jax.experimental import pallas as pl
from jax.experimental.pallas import tpu as pltpu
from jax.sharding import Mesh
from jax.sharding import PartitionSpec as P


NZ, NY, NX = 8, 4, 4
RING = 4
BLOCK = 176
COLS = 3 * BLOCK
HALF = 128
ROWS = NY * HALF
SWAP = [(0, 1), (1, 0)]
ORDER = (0, -1, 1, 2)
VMEM = pl.BlockSpec(memory_space=pltpu.VMEM)
SMEM = pl.BlockSpec(memory_space=pltpu.SMEM)


def dot(left, right, dims):
    return lax.dot_general(
        left, right, (dims, ((), ())), preferred_element_type=jnp.float32
    )


def call(kernel, outs, specs, *args, dtype=jnp.bfloat16, scratch=()):
    return pl.pallas_call(
        kernel,
        out_shape=[jax.ShapeDtypeStruct(s, dtype) for s in outs],
        in_specs=specs,
        out_specs=[VMEM] * len(outs),
        scratch_shapes=[pltpu.VMEM(s, jnp.bfloat16) for s in scratch],
        compiler_params=pltpu.CompilerParams(vmem_limit_bytes=24 * 1024 * 1024),
    )(*args)


def shift(array, axis, by):
    return lax.ppermute(array, axis, [(i, (i + by) % RING) for i in range(RING)])


def around(own, axis):
    return own, shift(own, axis, 1), shift(own, axis, -1), shift(own, axis, 2)


def around_in_halves(own, axis):
    low, high = shift(own, axis, 1), shift(own, axis, -1)
    far_first = shift(low[:2], axis, 1)
    far_last = shift(high[2:], axis, -1)
    return own, low, high, far_first, far_last


def cut_kernel(place, gate, up, down, keep, to_next, to_prev, to_far, pieces):
    for y in range(NY):
        for part, array in enumerate((gate, up, down)):
            pieces[y, :, part * BLOCK : (part + 1) * BLOCK] = array[
                :, y * BLOCK : (y + 1) * BLOCK
            ]
    for out, by in ((keep, 0), (to_next, 1), (to_prev, NY - 1), (to_far, 2)):
        out[...] = pieces[(place[0] + by) % NY]


def pair_kernel(place, inputs, cotangent, came, inp, cot):
    for core in range(2):

        @pl.when(place[2] == core)
        def _():
            own = slice(core * 256, (core + 1) * 256)
            other = slice((1 - core) * 256, (2 - core) * 256)
            for which, (array, out) in enumerate(((inputs, inp), (cotangent, cot))):
                out[:, own] = array[core * HALF : (core + 1) * HALF, :]
                out[:, other] = came[which]


def join_kernel(place, kept, from_prev, from_next, from_far, out, pieces):
    for array, by in ((kept, 0), (from_prev, NY - 1), (from_next, 1), (from_far, 2)):
        pieces[(place[0] + by) % NY] = array[...]
    rows = jnp.concatenate([pieces[y] for y in range(NY)], axis=0)
    out[...] = rows.T


def split_kernel(place, grads, keep, to_next, to_prev, to_far, pieces):
    rows = grads[...].T
    for y in range(NY):
        pieces[y] = rows[y * 64 : (y + 1) * 64]
    for out, by in ((keep, 0), (to_next, 1), (to_prev, NY - 1), (to_far, 2)):
        out[...] = pieces[(place[0] + by) % NY]


def finish_kernel(place, kept, from_prev, from_next, from_far, gate, up, down, pieces):
    for array, by in ((kept, 0), (from_prev, NY - 1), (from_next, 1), (from_far, 2)):
        pieces[(place[0] + by) % NY] = array[...]
    for y in range(NY):
        for part, out in enumerate((gate, up, down)):
            out[:, y * BLOCK : (y + 1) * BLOCK] = pieces[
                y, :, part * BLOCK : (part + 1) * BLOCK
            ].astype(jnp.float32)


def exchange(pieces):
    keep, to_next, to_prev, to_far = pieces
    return keep, shift(to_next, "y", 1), shift(to_prev, "y", -1), shift(to_far, "y", 2)


def main_kernel(place, *refs):
    inp, cot = refs[0:5], refs[5:10]
    weights = refs[10:12]
    hid, grads = refs[12], refs[13:15]
    columns = [(place[1] + by + NX) % NX for by in ORDER]

    def tile(which, y, x, lanes=slice(None)):
        arrays, near, far = (inp, x, y) if which == 0 else (cot, y, x)
        if far == 3:
            return arrays[3 + near // 2][near % 2, :, lanes]
        return arrays[far][near, :, lanes]

    def tall(first, last):
        return jnp.concatenate(
            [
                jnp.concatenate(
                    [array[2 * x + side, first:last, :] for x in columns for side in range(2)],
                    axis=1,
                )
                for array in weights
            ],
            axis=0,
        )

    for half in range(2):
        rows = slice(half * 256, (half + 1) * 256)

        def tokens(which):
            return jnp.concatenate(
                [
                    jnp.concatenate([tile(which, y, x) for x in range(NX)], axis=1)
                    for y in (2 * half, 2 * half + 1)
                ],
                axis=0,
            )

        pre = dot(tall(0, 2 * BLOCK), tokens(0), ((1,), (1,)))
        back = dot(tall(2 * BLOCK, COLS), tokens(1), ((1,), (1,)))
        for block in range(2):
            at = block * 2 * BLOCK
            gate_pre, up_pre = pre[at : at + BLOCK], pre[at + BLOCK : at + 2 * BLOCK]
            grad_hidden = back[block * BLOCK : (block + 1) * BLOCK]
            gate_sig = jax.nn.sigmoid(gate_pre)
            gate_act = gate_pre * gate_sig
            hid[at : at + BLOCK, rows] = (
                grad_hidden * up_pre * gate_sig * (1.0 + gate_pre * (1.0 - gate_sig))
            ).astype(jnp.bfloat16)
            hid[at + BLOCK : at + 2 * BLOCK, rows] = (grad_hidden * gate_act).astype(jnp.bfloat16)
            hid[4 * BLOCK + block * BLOCK : 4 * BLOCK + (block + 1) * BLOCK, rows] = (
                gate_act * up_pre
            ).astype(jnp.bfloat16)
    for slot, x in enumerate(columns):
        for side in range(2):
            lanes = slice(side * 256, (side + 1) * 256)
            for which, rows, first, size in ((0, 0, 0, 2 * BLOCK), (1, 4 * BLOCK, 2 * BLOCK, BLOCK)):
                acts = jnp.concatenate([tile(which, y, slot, lanes) for y in range(NY)], axis=0)
                grad = dot(hid[rows : rows + 2 * size], acts, ((1,), (0,))).astype(jnp.bfloat16)
                for block in range(2):
                    grads[block][2 * x + side, first : first + size, :] = grad[
                        block * size : (block + 1) * size
                    ]


def inputs_kernel(place, hid, weights_a, weights_b, out, flipped):
    flipped[...] = hid[0 : 4 * BLOCK, :].T
    for z in range(NZ):
        rows = jnp.concatenate([weights_a[z, : 2 * BLOCK], weights_b[z, : 2 * BLOCK]], axis=0)
        total = dot(flipped[...], rows, ((1,), (0,))).astype(jnp.bfloat16)
        lanes = slice((z % 2) * 256, (z % 2 + 1) * 256)
        for slot in range(NY):
            y = (place[0] + ORDER[slot] + NY) % NY
            out[y * NX + z // 2, :, lanes] = total[slot * HALF : (slot + 1) * HALF]


def per_device(inputs, cotangent, gate_weight, up_weight, down_weight):
    core = lax.axis_index("core")
    place = jnp.stack([lax.axis_index("y"), lax.axis_index("x"), core]).astype(jnp.int32)

    both = jnp.stack([inputs, cotangent]).reshape(2, 2, HALF, 256)
    sent = jnp.where(core == 0, both[:, 1], both[:, 0])
    came = lax.ppermute(sent, "core", SWAP)

    piece = (64, COLS)
    pieces = call(
        cut_kernel,
        [piece] * 4,
        [SMEM] + [VMEM] * 3,
        place,
        gate_weight,
        up_weight,
        down_weight.T,
        scratch=[(NY, *piece)],
    )
    moved = exchange(pieces)
    (rows,) = call(
        join_kernel,
        [(COLS, 256)],
        [SMEM] + [VMEM] * 4,
        place,
        *moved,
        scratch=[(NY, *piece)],
    )
    w_own = lax.all_gather(rows, "z", axis=0, tiled=False)

    inp, cot = call(
        pair_kernel, [(HALF, 512)] * 2, [SMEM] + [VMEM] * 3, place, inputs, cotangent, came
    )
    inp_near, cot_near = around(inp, "x"), around(cot, "y")
    inp_blocks = around_in_halves(jnp.stack(inp_near), "y")
    cot_blocks = around_in_halves(jnp.stack(cot_near), "x")

    w_other = lax.ppermute(w_own, "core", SWAP)

    grads_shape = (NZ, COLS, 256)
    hid_shape = (2 * COLS, ROWS)
    hid, grads_other, grads_own = call(
        main_kernel,
        [hid_shape, grads_shape, grads_shape],
        [SMEM] + [VMEM] * 12,
        place,
        *inp_blocks,
        *cot_blocks,
        w_other,
        w_own,
    )
    grads_came = lax.ppermute(grads_other, "core", SWAP)
    (partial,) = call(
        inputs_kernel,
        [(NY * NX, HALF, 512)],
        [SMEM] + [VMEM] * 3,
        place,
        hid,
        w_other,
        w_own,
        scratch=[(ROWS, 4 * BLOCK)],
    )
    grads = grads_own.astype(jnp.float32) + grads_came.astype(jnp.float32)
    grads = grads.astype(jnp.bfloat16)

    summed = lax.psum_scatter(grads, "z", scatter_dimension=0, tiled=False)
    pieces = call(
        split_kernel, [piece] * 4, [SMEM, VMEM], place, summed, scratch=[(NY, *piece)]
    )
    grad_gate, grad_up, grad_down = call(
        finish_kernel,
        [(64, NY * BLOCK)] * 3,
        [SMEM] + [VMEM] * 4,
        place,
        *exchange(pieces),
        dtype=jnp.float32,
        scratch=[(NY, *piece)],
    )

    arrived = lax.all_to_all(partial, ("y", "x"), split_axis=0, concat_axis=0, tiled=True)
    total = arrived.astype(jnp.float32).sum(axis=0).astype(jnp.bfloat16)
    lower, upper = total[:, :256], total[:, 256:]
    keep, give = jnp.where(core == 0, lower, upper), jnp.where(core == 0, upper, lower)
    take = lax.ppermute(give, "core", SWAP)
    grad_inputs = jnp.concatenate(
        [jnp.where(core == 0, keep, take), jnp.where(core == 0, take, keep)], axis=0
    )
    return grad_inputs, grad_gate, grad_up, grad_down.T


def solution(mesh):
    finer = Mesh(mesh.devices.reshape(NZ, NY, NX, 2), ("z", "y", "x", "core"))
    fs, tp = ("z", "y"), ("x", "core")

    return jax.shard_map(
        per_device,
        mesh=finer,
        in_specs=(P(fs, tp), P(fs, tp), P(fs, tp), P(fs, tp), P(tp, fs)),
        out_specs=(P(fs, tp), P(fs, tp), P(fs, tp), P(tp, fs)),
        check_vma=False,
    )
```

```python
import jax
import jax.numpy as jnp
from jax import lax
from jax.experimental import pallas as pl
from jax.experimental.pallas import tpu as pltpu
from jax.sharding import Mesh
from jax.sharding import PartitionSpec as P


NZ, NY, NX = 8, 4, 4
RING = 4
BLOCK = 176
COLS = 3 * BLOCK
HALF = 128
ROWS = NY * HALF
SWAP = [(0, 1), (1, 0)]
ORDER = (0, -1, 1, 2)
VMEM = pl.BlockSpec(memory_space=pltpu.VMEM)
SMEM = pl.BlockSpec(memory_space=pltpu.SMEM)


def dot(left, right, dims):
    return lax.dot_general(
        left, right, (dims, ((), ())), preferred_element_type=jnp.float32
    )


def call(kernel, outs, specs, *args, dtype=jnp.bfloat16, scratch=()):
    return pl.pallas_call(
        kernel,
        out_shape=[jax.ShapeDtypeStruct(s, dtype) for s in outs],
        in_specs=specs,
        out_specs=[VMEM] * len(outs),
        scratch_shapes=[pltpu.VMEM(s, jnp.bfloat16) for s in scratch],
        compiler_params=pltpu.CompilerParams(vmem_limit_bytes=24 * 1024 * 1024),
    )(*args)


def shift(array, axis, by):
    return lax.ppermute(array, axis, [(i, (i + by) % RING) for i in range(RING)])


def around(own, axis):
    return own, shift(own, axis, 1), shift(own, axis, -1), shift(own, axis, 2)


def around_in_halves(own, axis):
    low, high = shift(own, axis, 1), shift(own, axis, -1)
    far_first = shift(low[:2], axis, 1)
    far_last = shift(high[2:], axis, -1)
    return own, low, high, far_first, far_last


def cut_kernel(place, gate, up, down, keep, to_next, to_prev, to_far, pieces):
    for y in range(NY):
        for part, array in enumerate((gate, up, down)):
            pieces[y, :, part * BLOCK : (part + 1) * BLOCK] = array[
                :, y * BLOCK : (y + 1) * BLOCK
            ]
    for out, by in ((keep, 0), (to_next, 1), (to_prev, NY - 1), (to_far, 2)):
        out[...] = pieces[(place[0] + by) % NY]


def pair_kernel(place, inputs, cotangent, came, inp, cot):
    for core in range(2):

        @pl.when(place[2] == core)
        def _():
            own = slice(core * 256, (core + 1) * 256)
            other = slice((1 - core) * 256, (2 - core) * 256)
            for which, (array, out) in enumerate(((inputs, inp), (cotangent, cot))):
                out[:, own] = array[core * HALF : (core + 1) * HALF, :]
                out[:, other] = came[which]


def join_kernel(place, kept, from_prev, from_next, from_far, out, pieces):
    for array, by in ((kept, 0), (from_prev, NY - 1), (from_next, 1), (from_far, 2)):
        pieces[(place[0] + by) % NY] = array[...]
    rows = jnp.concatenate([pieces[y] for y in range(NY)], axis=0)
    out[...] = rows.T


def split_kernel(place, grads, keep, to_next, to_prev, to_far, pieces):
    rows = grads[...].T
    for y in range(NY):
        pieces[y] = rows[y * 64 : (y + 1) * 64]
    for out, by in ((keep, 0), (to_next, 1), (to_prev, NY - 1), (to_far, 2)):
        out[...] = pieces[(place[0] + by) % NY]


def finish_kernel(place, kept, from_prev, from_next, from_far, gate, up, down, pieces):
    for array, by in ((kept, 0), (from_prev, NY - 1), (from_next, 1), (from_far, 2)):
        pieces[(place[0] + by) % NY] = array[...]
    for y in range(NY):
        for part, out in enumerate((gate, up, down)):
            out[:, y * BLOCK : (y + 1) * BLOCK] = pieces[
                y, :, part * BLOCK : (part + 1) * BLOCK
            ].astype(jnp.float32)


def exchange(pieces):
    keep, to_next, to_prev, to_far = pieces
    return keep, shift(to_next, "y", 1), shift(to_prev, "y", -1), shift(to_far, "y", 2)


def block_kernel(place, *refs):
    inp, cot = refs[0:5], refs[5:10]
    weights, hid, grads = refs[10:13]
    columns = [(place[1] + by + NX) % NX for by in ORDER]

    def tile(which, y, x, lanes=slice(None)):
        arrays, near, far = (inp, x, y) if which == 0 else (cot, y, x)
        if far == 3:
            return arrays[3 + near // 2][near % 2, :, lanes]
        return arrays[far][near, :, lanes]

    def wide(first, last):
        return jnp.concatenate(
            [weights[2 * x + side, first:last, :] for x in columns for side in range(2)], axis=1
        )

    for half in range(2):
        rows = slice(half * 256, (half + 1) * 256)

        def tokens(which):
            return jnp.concatenate(
                [
                    jnp.concatenate([tile(which, y, x) for x in range(NX)], axis=1)
                    for y in (2 * half, 2 * half + 1)
                ],
                axis=0,
            )

        pre = dot(wide(0, 2 * BLOCK), tokens(0), ((1,), (1,)))
        grad_hidden = dot(wide(2 * BLOCK, COLS), tokens(1), ((1,), (1,)))
        gate_pre, up_pre = pre[:BLOCK], pre[BLOCK:]
        gate_sig = jax.nn.sigmoid(gate_pre)
        gate_act = gate_pre * gate_sig
        hid[0:BLOCK, rows] = (
            grad_hidden * up_pre * gate_sig * (1.0 + gate_pre * (1.0 - gate_sig))
        ).astype(jnp.bfloat16)
        hid[BLOCK : 2 * BLOCK, rows] = (grad_hidden * gate_act).astype(jnp.bfloat16)
        hid[2 * BLOCK : COLS, rows] = (gate_act * up_pre).astype(jnp.bfloat16)
    for slot, x in enumerate(columns):
        for side in range(2):
            lanes = slice(side * 256, (side + 1) * 256)
            for which, rows in ((0, slice(0, 2 * BLOCK)), (1, slice(2 * BLOCK, COLS))):
                acts = jnp.concatenate([tile(which, y, slot, lanes) for y in range(NY)], axis=0)
                grads[2 * x + side, rows, :] = dot(hid[rows], acts, ((1,), (0,))).astype(
                    jnp.bfloat16
                )


def inputs_kernel(place, hid_a, hid_b, weights_a, weights_b, out, flipped):
    both = jnp.concatenate([hid_a[: 2 * BLOCK], hid_b[: 2 * BLOCK]], axis=0)
    flipped[...] = both.T
    for z in range(NZ):
        rows = jnp.concatenate([weights_a[z, : 2 * BLOCK], weights_b[z, : 2 * BLOCK]], axis=0)
        total = dot(flipped[...], rows, ((1,), (0,))).astype(jnp.bfloat16)
        lanes = slice((z % 2) * 256, (z % 2 + 1) * 256)
        for slot in range(NY):
            y = (place[0] + ORDER[slot] + NY) % NY
            out[y * NX + z // 2, :, lanes] = total[slot * HALF : (slot + 1) * HALF]


def per_device(inputs, cotangent, gate_weight, up_weight, down_weight):
    core = lax.axis_index("core")
    place = jnp.stack([lax.axis_index("y"), lax.axis_index("x"), core]).astype(jnp.int32)

    both = jnp.stack([inputs, cotangent]).reshape(2, 2, HALF, 256)
    sent = jnp.where(core == 0, both[:, 1], both[:, 0])
    came = lax.ppermute(sent, "core", SWAP)

    piece = (64, COLS)
    pieces = call(
        cut_kernel,
        [piece] * 4,
        [SMEM] + [VMEM] * 3,
        place,
        gate_weight,
        up_weight,
        down_weight.T,
        scratch=[(NY, *piece)],
    )
    moved = exchange(pieces)
    (rows,) = call(
        join_kernel,
        [(COLS, 256)],
        [SMEM] + [VMEM] * 4,
        place,
        *moved,
        scratch=[(NY, *piece)],
    )
    w_own = lax.all_gather(rows, "z", axis=0, tiled=False)

    inp, cot = call(
        pair_kernel, [(HALF, 512)] * 2, [SMEM] + [VMEM] * 3, place, inputs, cotangent, came
    )
    inp_near, cot_near = around(inp, "x"), around(cot, "y")
    inp_blocks = around_in_halves(jnp.stack(inp_near), "y")
    cot_blocks = around_in_halves(jnp.stack(cot_near), "x")

    w_other = lax.ppermute(w_own, "core", SWAP)

    def block(weights):
        return call(
            block_kernel,
            [(COLS, ROWS), (NZ, COLS, 256)],
            [SMEM] + [VMEM] * 11,
            place,
            *inp_blocks,
            *cot_blocks,
            weights,
        )

    hid_own, grads_own = block(w_own)
    hid_other, grads_other = block(w_other)
    grads_came = lax.ppermute(grads_other, "core", SWAP)
    (partial,) = call(
        inputs_kernel,
        [(NY * NX, HALF, 512)],
        [SMEM] + [VMEM] * 4,
        place,
        hid_other,
        hid_own,
        w_other,
        w_own,
        scratch=[(ROWS, 4 * BLOCK)],
    )
    grads = grads_own.astype(jnp.float32) + grads_came.astype(jnp.float32)
    grads = grads.astype(jnp.bfloat16)

    summed = lax.psum_scatter(grads, "z", scatter_dimension=0, tiled=False)
    pieces = call(
        split_kernel, [piece] * 4, [SMEM, VMEM], place, summed, scratch=[(NY, *piece)]
    )
    grad_gate, grad_up, grad_down = call(
        finish_kernel,
        [(64, NY * BLOCK)] * 3,
        [SMEM] + [VMEM] * 4,
        place,
        *exchange(pieces),
        dtype=jnp.float32,
        scratch=[(NY, *piece)],
    )

    arrived = lax.all_to_all(partial, ("y", "x"), split_axis=0, concat_axis=0, tiled=True)
    total = arrived.astype(jnp.float32).sum(axis=0).astype(jnp.bfloat16)
    lower, upper = total[:, :256], total[:, 256:]
    keep, give = jnp.where(core == 0, lower, upper), jnp.where(core == 0, upper, lower)
    take = lax.ppermute(give, "core", SWAP)
    grad_inputs = jnp.concatenate(
        [jnp.where(core == 0, keep, take), jnp.where(core == 0, take, keep)], axis=0
    )
    return grad_inputs, grad_gate, grad_up, grad_down.T


def solution(mesh):
    finer = Mesh(mesh.devices.reshape(NZ, NY, NX, 2), ("z", "y", "x", "core"))
    fs, tp = ("z", "y"), ("x", "core")

    return jax.shard_map(
        per_device,
        mesh=finer,
        in_specs=(P(fs, tp), P(fs, tp), P(fs, tp), P(fs, tp), P(tp, fs)),
        out_specs=(P(fs, tp), P(fs, tp), P(fs, tp), P(tp, fs)),
        check_vma=False,
    )
```

```python
import jax
import jax.numpy as jnp
from jax import lax
from jax.experimental import pallas as pl
from jax.experimental.pallas import tpu as pltpu
from jax.sharding import Mesh
from jax.sharding import PartitionSpec as P


NZ, NY, NX = 8, 4, 4
RING = 4
BLOCK = 176
COLS = 3 * BLOCK
HALF = 128
ROWS = NY * HALF
SWAP = [(0, 1), (1, 0)]
ORDER = (0, -1, 1, 2)
VMEM = pl.BlockSpec(memory_space=pltpu.VMEM)
ANY = pl.BlockSpec(memory_space=pl.ANY)
SMEM = pl.BlockSpec(memory_space=pltpu.SMEM)


def dot(left, right, dims):
    return lax.dot_general(
        left, right, (dims, ((), ())), preferred_element_type=jnp.float32
    )


def call(kernel, outs, specs, *args, dtype=jnp.bfloat16, scratch=()):
    return pl.pallas_call(
        kernel,
        out_shape=[jax.ShapeDtypeStruct(s, dtype) for s in outs],
        in_specs=specs,
        out_specs=[VMEM] * len(outs),
        scratch_shapes=[pltpu.VMEM(s, jnp.bfloat16) for s in scratch],
        compiler_params=pltpu.CompilerParams(vmem_limit_bytes=24 * 1024 * 1024),
    )(*args)


def shift(array, axis, by):
    return lax.ppermute(array, axis, [(i, (i + by) % RING) for i in range(RING)])


def around(own, axis):
    return own, shift(own, axis, 1), shift(own, axis, -1), shift(own, axis, 2)


def around_in_halves(own, axis):
    low, high = shift(own, axis, 1), shift(own, axis, -1)
    far_first = shift(low[:2], axis, 1)
    far_last = shift(high[2:], axis, -1)
    return own, low, high, far_first, far_last


def cut_kernel(place, gate, up, down, keep, to_next, to_prev, to_far, pieces):
    for y in range(NY):
        for part, array in enumerate((gate, up, down)):
            pieces[y, :, part * BLOCK : (part + 1) * BLOCK] = array[
                :, y * BLOCK : (y + 1) * BLOCK
            ]
    for out, by in ((keep, 0), (to_next, 1), (to_prev, NY - 1), (to_far, 2)):
        out[...] = pieces[(place[0] + by) % NY]


def pair_kernel(place, inputs, cotangent, came, inp, cot):
    for core in range(2):

        @pl.when(place[2] == core)
        def _():
            own = slice(core * 256, (core + 1) * 256)
            other = slice((1 - core) * 256, (2 - core) * 256)
            for which, (array, out) in enumerate(((inputs, inp), (cotangent, cot))):
                out[:, own] = array[core * HALF : (core + 1) * HALF, :]
                out[:, other] = came[which]


def join_kernel(place, kept, from_prev, from_next, from_far, out, pieces):
    for array, by in ((kept, 0), (from_prev, NY - 1), (from_next, 1), (from_far, 2)):
        pieces[(place[0] + by) % NY] = array[...]
    rows = jnp.concatenate([pieces[y] for y in range(NY)], axis=0)
    out[...] = rows.T


def split_kernel(place, grads, keep, to_next, to_prev, to_far, pieces):
    rows = grads[...].T
    for y in range(NY):
        pieces[y] = rows[y * 64 : (y + 1) * 64]
    for out, by in ((keep, 0), (to_next, 1), (to_prev, NY - 1), (to_far, 2)):
        out[...] = pieces[(place[0] + by) % NY]


def finish_kernel(place, kept, from_prev, from_next, from_far, gate, up, down, pieces):
    for array, by in ((kept, 0), (from_prev, NY - 1), (from_next, 1), (from_far, 2)):
        pieces[(place[0] + by) % NY] = array[...]
    for y in range(NY):
        for part, out in enumerate((gate, up, down)):
            out[:, y * BLOCK : (y + 1) * BLOCK] = pieces[
                y, :, part * BLOCK : (part + 1) * BLOCK
            ].astype(jnp.float32)


def exchange(pieces):
    keep, to_next, to_prev, to_far = pieces
    return keep, shift(to_next, "y", 1), shift(to_prev, "y", -1), shift(to_far, "y", 2)


def block_kernel(place, *refs):
    inp, cot = refs[0:5], refs[5:10]
    weights, hid, grads = refs[10:13]
    columns = [(place[1] + by + NX) % NX for by in ORDER]

    def tile(which, y, x, lanes=slice(None)):
        arrays, near, far = (inp, x, y) if which == 0 else (cot, y, x)
        if far == 3:
            return arrays[3 + near // 2][near % 2, :, lanes]
        return arrays[far][near, :, lanes]

    def wide(first, last):
        return jnp.concatenate(
            [weights[2 * x + side, first:last, :] for x in columns for side in range(2)], axis=1
        )

    for half in range(2):
        rows = slice(half * 256, (half + 1) * 256)

        def tokens(which):
            return jnp.concatenate(
                [
                    jnp.concatenate([tile(which, y, x) for x in range(NX)], axis=1)
                    for y in (2 * half, 2 * half + 1)
                ],
                axis=0,
            )

        pre = dot(wide(0, 2 * BLOCK), tokens(0), ((1,), (1,)))
        grad_hidden = dot(wide(2 * BLOCK, COLS), tokens(1), ((1,), (1,)))
        gate_pre, up_pre = pre[:BLOCK], pre[BLOCK:]
        gate_sig = jax.nn.sigmoid(gate_pre)
        gate_act = gate_pre * gate_sig
        hid[0:BLOCK, rows] = (
            grad_hidden * up_pre * gate_sig * (1.0 + gate_pre * (1.0 - gate_sig))
        ).astype(jnp.bfloat16)
        hid[BLOCK : 2 * BLOCK, rows] = (grad_hidden * gate_act).astype(jnp.bfloat16)
        hid[2 * BLOCK : COLS, rows] = (gate_act * up_pre).astype(jnp.bfloat16)
    for slot, x in enumerate(columns):
        for side in range(2):
            lanes = slice(side * 256, (side + 1) * 256)
            for which, rows in ((0, slice(0, 2 * BLOCK)), (1, slice(2 * BLOCK, COLS))):
                acts = jnp.concatenate([tile(which, y, slot, lanes) for y in range(NY)], axis=0)
                grads[2 * x + side, rows, :] = dot(hid[rows], acts, ((1,), (0,))).astype(
                    jnp.bfloat16
                )


def inputs_kernel(place, hid_a, hid_b, weights_a, weights_b, out, flipped):
    both = jnp.concatenate([hid_a[: 2 * BLOCK], hid_b[: 2 * BLOCK]], axis=0)
    flipped[...] = both.T
    for z in range(NZ):
        rows = jnp.concatenate([weights_a[z, : 2 * BLOCK], weights_b[z, : 2 * BLOCK]], axis=0)
        total = dot(flipped[...], rows, ((1,), (0,))).astype(jnp.bfloat16)
        lanes = slice((z % 2) * 256, (z % 2 + 1) * 256)
        for slot in range(NY):
            y = (place[0] + ORDER[slot] + NY) % NY
            out[y * NX + z // 2, :, lanes] = total[slot * HALF : (slot + 1) * HALF]


def fetch_kernel(held, out, sem):
    copy = pltpu.make_async_copy(held, out, sem)
    copy.start()
    copy.wait()


def per_device(inputs, cotangent, gate_weight, up_weight, down_weight):
    core = lax.axis_index("core")
    place = jnp.stack([lax.axis_index("y"), lax.axis_index("x"), core]).astype(jnp.int32)

    both = jnp.stack([inputs, cotangent]).reshape(2, 2, HALF, 256)
    sent = jnp.where(core == 0, both[:, 1], both[:, 0])
    came = lax.ppermute(sent, "core", SWAP)

    piece = (64, COLS)
    pieces = call(
        cut_kernel,
        [piece] * 4,
        [SMEM] + [VMEM] * 3,
        place,
        gate_weight,
        up_weight,
        down_weight.T,
        scratch=[(NY, *piece)],
    )
    moved = exchange(pieces)
    (rows,) = call(
        join_kernel,
        [(COLS, 256)],
        [SMEM] + [VMEM] * 4,
        place,
        *moved,
        scratch=[(NY, *piece)],
    )
    w_own = lax.all_gather(rows, "z", axis=0, tiled=False)

    inp, cot = call(
        pair_kernel, [(HALF, 512)] * 2, [SMEM] + [VMEM] * 3, place, inputs, cotangent, came
    )
    inp_near, cot_near = around(inp, "x"), around(cot, "y")
    inp_blocks = around_in_halves(jnp.stack(inp_near), "y")
    cot_blocks = around_in_halves(jnp.stack(cot_near), "x")

    w_own = pl.pallas_call(
        fetch_kernel,
        out_shape=jax.ShapeDtypeStruct((NZ, COLS, 256), jnp.bfloat16),
        in_specs=[ANY],
        out_specs=VMEM,
        scratch_shapes=[pltpu.SemaphoreType.DMA],
        compiler_params=pltpu.CompilerParams(vmem_limit_bytes=24 * 1024 * 1024),
    )(w_own)
    w_other = lax.ppermute(w_own, "core", SWAP)

    def block(weights):
        return call(
            block_kernel,
            [(COLS, ROWS), (NZ, COLS, 256)],
            [SMEM] + [VMEM] * 11,
            place,
            *inp_blocks,
            *cot_blocks,
            weights,
        )

    hid_own, grads_own = block(w_own)
    hid_other, grads_other = block(w_other)
    grads_came = lax.ppermute(grads_other, "core", SWAP)
    (partial,) = call(
        inputs_kernel,
        [(NY * NX, HALF, 512)],
        [SMEM] + [VMEM] * 4,
        place,
        hid_other,
        hid_own,
        w_other,
        w_own,
        scratch=[(ROWS, 4 * BLOCK)],
    )
    grads = grads_own.astype(jnp.float32) + grads_came.astype(jnp.float32)
    grads = grads.astype(jnp.bfloat16)

    summed = lax.psum_scatter(grads, "z", scatter_dimension=0, tiled=False)
    pieces = call(
        split_kernel, [piece] * 4, [SMEM, VMEM], place, summed, scratch=[(NY, *piece)]
    )
    grad_gate, grad_up, grad_down = call(
        finish_kernel,
        [(64, NY * BLOCK)] * 3,
        [SMEM] + [VMEM] * 4,
        place,
        *exchange(pieces),
        dtype=jnp.float32,
        scratch=[(NY, *piece)],
    )

    arrived = lax.all_to_all(partial, ("y", "x"), split_axis=0, concat_axis=0, tiled=True)
    total = arrived.astype(jnp.float32).sum(axis=0).astype(jnp.bfloat16)
    lower, upper = total[:, :256], total[:, 256:]
    keep, give = jnp.where(core == 0, lower, upper), jnp.where(core == 0, upper, lower)
    take = lax.ppermute(give, "core", SWAP)
    grad_inputs = jnp.concatenate(
        [jnp.where(core == 0, keep, take), jnp.where(core == 0, take, keep)], axis=0
    )
    return grad_inputs, grad_gate, grad_up, grad_down.T


def solution(mesh):
    finer = Mesh(mesh.devices.reshape(NZ, NY, NX, 2), ("z", "y", "x", "core"))
    fs, tp = ("z", "y"), ("x", "core")

    return jax.shard_map(
        per_device,
        mesh=finer,
        in_specs=(P(fs, tp), P(fs, tp), P(fs, tp), P(fs, tp), P(tp, fs)),
        out_specs=(P(fs, tp), P(fs, tp), P(fs, tp), P(tp, fs)),
        check_vma=False,
    )
```
